32 devices in a mesh: grp: 2 (over y), sp: 4 (over z), tp: 4 (over x, core).
Axes of the slice: x: 2, y: 2, z: 4, core: 2. Of those that a mesh axis runs over, the one named last changes fastest.
Arguments:
- stream: bfloat16 [2048, 2048], P(('grp', 'sp')), parts along dimension 0, may hold values from -6 to 6
- doc_ids: int32 [2048], P(('grp', 'sp')), parts along dimension 0, may hold values from 0 to 1, never falling along the last dimension, each value on 1 to 768 neighbouring positions
- norm_gain: float32 [2, 2048], replicated, may hold values from 0.1 to 1.9
- query_weight: bfloat16 [2, 2048, 1024], P(None, 'sp', 'tp'), may hold values from -0.125 to 0.125
- key_weight: bfloat16 [2, 2048, 1024], P(None, 'sp', 'tp'), may hold values from -0.125 to 0.125
- value_weight: bfloat16 [2, 2048, 1024], P(None, 'sp', 'tp'), may hold values from -0.125 to 0.125
- out_weight: bfloat16 [2, 1024, 2048], P(None, 'sp', 'tp'), may hold values from -0.75 to 0.75
- query_gain: float32 [2, 64], replicated, may hold values from 0.1 to 1.9
- key_gain: float32 [2, 64], replicated, may hold values from 0.1 to 1.9
- rel_bias: float32 [16, 513], P('tp'), may hold values from -4 to 250
Outputs:
- encoded: bfloat16 [2048, 2048], P(('grp', 'sp')), parts along dimension 0
The draws below stay inside these ranges and needn't reach their ends.
There are 2 independent parts, one for each index of `grp`. The reference program is written for one: setup_inputs(seed, part) draws one part's arguments, and reference() takes and returns one part's arrays. A program takes and returns all parts, laid end to end along the dimension named above; an argument that names none is the same for every part. Nothing has to cross between parts.
Inputs may be any that keep to these rules, and one draw needn't show every extreme that they name: doc_ids never fall along the sequence; each document has at most 768 positions.
All inputs are finite; a program needn't handle non-finite values.
Results may differ from the reference program's by a relative error of at most 0.011.
Values may be sent and summed in bfloat16 or wider, within the bound.
No kernel may reach another device: no remote copies, remote signals or barrier semaphores. Data moves between devices by JAX's collectives and lax.ppermute only.
A program may use at most 64 MiB of HBM per device.

```python
import math
import jax
import jax.numpy as jnp
import numpy as np
from jax import lax

D = 2048
HEADS = 16
HD = 64
DA = 1024
SEG = 64
LEFT = 8
MAXREL = 256
NREL = 513
LAYERS = 2
TOK_DEV = 256
TOKENS = 1024
DOCS = 2


def draw_rel_bias(key, part):
    base_key = jax.random.fold_in(key, 11)
    table = jnp.clip(jax.random.normal(base_key, (HEADS, NREL), jnp.float32), -4.0, 4.0)
    return table


def block_scale(rng, extent, shards, least, high):
    def one(position, blocks):
        heights = jax.random.uniform(jax.random.fold_in(jax.random.fold_in(rng, 6), position), (blocks,), jnp.float32, least / len(shards), high / len(shards))
        return jnp.repeat(jnp.exp(heights), extent[position] // blocks).reshape((-1,) + (1,) * (len(extent) - position - 1))

    level = one(*shards[0])
    for cut in shards[1:]:
        level = level * one(*cut)
    return level


def profile(amount, total, most, skew):
    weights = [(1 << 20) // math.isqrt(standing ** skew) + 1 for standing in range(2, amount + 1)]
    rest, holding = total - most - (amount - 1), [1] * (amount - 1)
    while rest > 0:
        candidates = [i for i in range(amount - 1) if holding[i] < most]
        whole, left = sum([weights[i] for i in candidates]), rest
        for i in candidates:
            extra = min(most - holding[i], max(1, left * weights[i] // whole), rest)
            holding[i] = holding[i] + extra
            rest = rest - extra
    return np.array([most] + holding)


def uneven_parts(own_key, count, total, bound, lean):
    if count == 2:
        one = jax.random.randint(own_key, (), max(1, total - bound), min(bound, total - 1) + 1)
        return jnp.stack([one, total - one])
    tallies = jnp.asarray(profile(count, total, bound, lean), jnp.int32)
    couples = (count - 1) // 2
    giver, taker = tallies[1:1 + 2 * couples:2], tallies[2:2 + 2 * couples:2]
    slack = jnp.minimum(giver - 1, bound - taker)
    shifted = jax.random.randint(jax.random.fold_in(own_key, 1), (couples,), 0, 1 << 20) % (slack + 1)
    tallies = tallies.at[1:1 + 2 * couples:2].set(giver - shifted).at[2:2 + 2 * couples:2].set(taker + shifted)
    return tallies[jax.random.permutation(jax.random.fold_in(own_key, 2), count)]


def noise(key, shape, scale, most, cuts=(), kind=jnp.bfloat16):
    values = scale * jax.random.normal(key, shape, jnp.float32)
    if cuts:
        values = values * block_scale(key, shape, cuts, -0.22, 0.18)
    return jnp.clip(values, -most, most).astype(kind)


def setup_inputs(seed: int = 0, part: int = 0) -> dict:
    key_of = jax.random.split(jax.random.key(seed), 11)
    part_splits = jax.random.split(jax.random.fold_in(key_of[10], part), 11)
    stream = noise(part_splits[0], (TOKENS, D), 1.0, 6.0, ((0, 4),))
    doc_ids = jnp.searchsorted(jnp.cumsum(uneven_parts(part_splits[1], DOCS, TOKENS, 3 * TOK_DEV, 1)), jnp.arange(TOKENS), side="right").astype(jnp.int32)
    norm_gain = jnp.clip(1.0 + 0.18 * jax.random.normal(key_of[2], (LAYERS, D), jnp.float32), 0.1, 1.9)
    query_weight = noise(key_of[3], (LAYERS, D, DA), D ** -0.5, 0.125, ((1, 4), (2, 4)))
    key_weight = noise(key_of[4], (LAYERS, D, DA), D ** -0.5, 0.125, ((1, 4), (2, 4)))
    value_weight = noise(key_of[5], (LAYERS, D, DA), D ** -0.5, 0.125, ((1, 4), (2, 4)))
    out_weight = noise(key_of[6], (LAYERS, DA, D), (DA // 16) ** -0.5, 0.75, ((1, 4), (2, 4)))
    query_gain = jnp.clip(1.0 + 0.18 * jax.random.normal(key_of[7], (LAYERS, HD), jnp.float32), 0.1, 1.9)
    key_gain = jnp.clip(1.0 + 0.18 * jax.random.normal(key_of[8], (LAYERS, HD), jnp.float32), 0.1, 1.9)
    rel_bias = draw_rel_bias(jax.random.fold_in(key_of[10], 71), part)
    return {"stream": stream, "doc_ids": doc_ids, "norm_gain": norm_gain, "query_weight": query_weight, "key_weight": key_weight, "value_weight": value_weight, "out_weight": out_weight, "query_gain": query_gain, "key_gain": key_gain, "rel_bias": rel_bias}


epsilon = 1e-06

def row_norm(values, gain):
    return values * lax.rsqrt(lax.optimization_barrier(jnp.mean(values * values, axis=-1, keepdims=True)) + epsilon) * gain

def band_of(values, count):
    blocks = values.reshape((count + LEFT, SEG) + values.shape[1:])
    stacked = jnp.stack([blocks[earlier:earlier + count] for earlier in range(LEFT + 1)], axis=1)
    return stacked.reshape((count, (LEFT + 1) * SEG) + values.shape[1:])

def reference(stream, doc_ids, norm_gain, query_weight, key_weight, value_weight, out_weight, query_gain, key_gain, rel_bias):
    total = stream.shape[0]
    count = total // SEG
    reach = LEFT * SEG
    width = (LEFT + 1) * SEG
    scale = HD ** (-0.5)
    distance = reach + jnp.arange(SEG, dtype=jnp.int32)[:, None] - jnp.arange(width, dtype=jnp.int32)[None, :]
    index = (jnp.clip(distance, -MAXREL, MAXREL) + MAXREL).astype(jnp.int32)
    table = jnp.take(rel_bias.astype(jnp.float32), index, axis=1)
    padded_docs = jnp.concatenate([jnp.full((reach,), -1, jnp.int32), doc_ids.astype(jnp.int32)])
    doc_band = band_of(padded_docs, count)
    key_pos = SEG * jnp.arange(count, dtype=jnp.int32)[:, None] - reach + jnp.arange(width, dtype=jnp.int32)[None, :]
    allowed = (key_pos >= 0)[:, None, :] & (doc_band[:, None, :] == doc_ids.reshape(count, SEG)[:, :, None])
    x = stream
    for layer in range(LAYERS):
        widened = x.astype(jnp.float32)
        normed = row_norm(widened, norm_gain[layer]).astype(jnp.bfloat16)
        q_raw = jnp.dot(normed, query_weight[layer], preferred_element_type=jnp.float32).reshape(total, HEADS, HD)
        k_raw = jnp.dot(normed, key_weight[layer], preferred_element_type=jnp.float32).reshape(total, HEADS, HD)
        v_raw = jnp.dot(normed, value_weight[layer], preferred_element_type=jnp.float32).reshape(total, HEADS, HD)
        query = row_norm(q_raw, query_gain[layer]).astype(jnp.bfloat16)
        keys = row_norm(k_raw, key_gain[layer]).astype(jnp.bfloat16)
        values = v_raw.astype(jnp.bfloat16)

        def one_head(operands):
            head_query, head_keys, head_values, head_table = operands
            pad_keys = jnp.concatenate([jnp.zeros((reach, HD), jnp.bfloat16), head_keys], axis=0)
            pad_values = jnp.concatenate([jnp.zeros((reach, HD), jnp.bfloat16), head_values], axis=0)
            key_band = band_of(pad_keys, count).astype(jnp.float32)
            value_band = band_of(pad_values, count).astype(jnp.float32)
            blocks = head_query.reshape(count, SEG, HD).astype(jnp.float32)
            scores = jnp.einsum('nqd,nkd->nqk', blocks, key_band) * scale + head_table[None]
            scores = jnp.where(allowed, scores, -1e+30)
            peak = lax.optimization_barrier(jnp.max(scores, axis=-1, keepdims=True))
            expo = jnp.exp(scores - peak)
            weights = (expo / lax.optimization_barrier(jnp.sum(expo, axis=-1, keepdims=True))).astype(jnp.bfloat16)
            mixed = jnp.einsum('nqk,nkd->nqd', weights.astype(jnp.float32), value_band)
            return mixed.astype(jnp.bfloat16).reshape(total, HD)
        attended = lax.map(one_head, (query.transpose(1, 0, 2), keys.transpose(1, 0, 2), values.transpose(1, 0, 2), table))
        attended = attended.transpose(1, 0, 2).reshape(total, HEADS * HD)
        x = (widened + jnp.dot(attended, out_weight[layer], preferred_element_type=jnp.float32)).astype(jnp.bfloat16)
    return x
```

```python
import jax
import jax.numpy as jnp
from jax import lax
from jax.experimental import pallas as pl
from jax.experimental.pallas import tpu as pltpu
from jax.sharding import PartitionSpec as P

SEG = 64
LEFT = 8
MAXREL = 256
LAYERS = 2


epsilon = 1e-06


def shifted(value, axis, steps):
    count = lax.axis_size(axis)
    initial, last = (max(0, -steps), min(count, count - steps))
    return lax.ppermute(value, axis, [(source, source + steps) for source in range(initial, last)])


def row_norm(values, gain):
    return values * lax.rsqrt(jnp.mean(values * values, axis=-1, keepdims=True) + epsilon) * gain


def bias_table(rel_bias):
    heads_here = rel_bias.shape[0]
    reach = LEFT * SEG
    width = (LEFT + 1) * SEG
    highest = reach + SEG - 1
    reversed_bias = rel_bias[:, ::-1]
    upper_fill = jnp.broadcast_to(rel_bias[:, -1:], (heads_here, highest - MAXREL))
    flat_row = jnp.concatenate([upper_fill, reversed_bias[:, : MAXREL + SEG]], axis=1)
    lines = [
        flat_row[:, SEG - 1 - position : SEG - 1 - position + width] for position in range(SEG)
    ]
    return jnp.stack(lines, axis=1)


def attend(query, ext_keys, ext_values, ext_docs, own_docs, offset, table):
    rows, heads_here, head_size = query.shape
    count = rows // SEG
    width = (LEFT + 1) * SEG
    blocks = query.reshape(count, SEG, heads_here, head_size)
    key_blocks = ext_keys.reshape(count + LEFT, SEG, heads_here, head_size)
    value_blocks = ext_values.reshape(count + LEFT, SEG, heads_here, head_size)
    doc_blocks = ext_docs.reshape(count + LEFT, SEG)
    score_parts = [
        jnp.einsum(
            "nqhd,nkhd->nhqk",
            blocks,
            key_blocks[earlier : earlier + count],
            preferred_element_type=jnp.float32,
        )
        for earlier in range(LEFT + 1)
    ]
    scores = jnp.concatenate(score_parts, axis=-1)
    scores = scores * head_size ** (-0.5) + table[None]
    doc_band = jnp.concatenate(
        [doc_blocks[earlier : earlier + count] for earlier in range(LEFT + 1)], axis=1
    )
    key_pos = (
        offset
        + SEG * jnp.arange(count, dtype=jnp.int32)[:, None]
        - LEFT * SEG
        + jnp.arange(width, dtype=jnp.int32)[None, :]
    )
    allowed = (key_pos >= 0)[:, None, None, :] & (
        doc_band[:, None, None, :] == own_docs.reshape(count, SEG)[:, None, :, None]
    )
    scores = jnp.where(allowed, scores, -1e30)
    peak = jnp.max(scores, axis=-1, keepdims=True)
    expo = jnp.exp(scores - peak)
    weights = (expo / jnp.sum(expo, axis=-1, keepdims=True)).astype(jnp.bfloat16)
    mixed = jnp.zeros((count, SEG, heads_here, head_size), jnp.float32)
    for earlier in range(LEFT + 1):
        part_weights = weights[..., earlier * SEG : (earlier + 1) * SEG]
        mixed = mixed + jnp.einsum(
            "nhqk,nkhd->nqhd",
            part_weights,
            value_blocks[earlier : earlier + count],
            preferred_element_type=jnp.float32,
        )
    return mixed.astype(jnp.bfloat16).reshape(rows, heads_here * head_size)


def on_device_general(
    stream,
    doc_ids,
    norm_gain,
    query_weight,
    key_weight,
    value_weight,
    out_weight,
    query_gain,
    key_gain,
    rel_bias,
):
    rows = stream.shape[0]
    heads_here = rel_bias.shape[0]
    head_size = query_gain.shape[1]
    local_width = heads_here * head_size
    reach = LEFT * SEG
    depth = -(-reach // rows)
    offset = lax.axis_index("sp") * rows
    col_width = out_weight.shape[2]
    col_start = lax.axis_index("tp") * col_width
    table = bias_table(rel_bias)
    x = stream
    for layer in range(LAYERS):
        widened = x.astype(jnp.float32)
        normed = row_norm(widened, norm_gain[layer]).astype(jnp.bfloat16)
        own_cols = normed
        q_raw = jnp.dot(
            own_cols,
            lax.all_gather(query_weight[layer], "sp", axis=0, tiled=True),
            preferred_element_type=jnp.float32,
        )
        k_raw = jnp.dot(
            normed,
            lax.all_gather(key_weight[layer], "sp", axis=0, tiled=True),
            preferred_element_type=jnp.float32,
        )
        v_raw = jnp.dot(
            normed,
            lax.all_gather(value_weight[layer], "sp", axis=0, tiled=True),
            preferred_element_type=jnp.float32,
        )
        query = row_norm(q_raw.reshape(rows, heads_here, head_size), query_gain[layer]).astype(
            jnp.bfloat16
        )
        keys = row_norm(
            k_raw.reshape(normed.shape[0], heads_here, head_size), key_gain[layer]
        ).astype(jnp.bfloat16)
        values = v_raw.astype(jnp.bfloat16)
        flat_keys = keys.reshape(rows, local_width)
        tail = (flat_keys, values, doc_ids)
        received = [
            shifted((tail[0], tail[1], tail[2]), "sp", distance_back)
            for distance_back in range(depth, 0, -1)
        ]
        ext_keys = jnp.concatenate([item[0] for item in received] + [flat_keys], axis=0)
        ext_values = jnp.concatenate([item[1] for item in received] + [values], axis=0)
        ext_docs = jnp.concatenate([item[2] for item in received] + [doc_ids], axis=0)
        ext_keys = ext_keys.reshape(reach + rows, heads_here, head_size)
        ext_values = ext_values.reshape(reach + rows, heads_here, head_size)
        attended = attend(query, ext_keys, ext_values, ext_docs, doc_ids, offset, table)
        all_heads = lax.all_gather(attended, "tp", axis=1, tiled=True)
        projected = jnp.dot(
            all_heads,
            lax.all_gather(out_weight[layer], "sp", axis=0, tiled=True),
            preferred_element_type=jnp.float32,
        )
        own_cols = lax.dynamic_slice_in_dim(widened, col_start, col_width, 1)
        new_cols = (own_cols + projected).astype(jnp.bfloat16)
        x = lax.all_gather(new_cols, "tp", axis=1, tiled=True)
    return x


VMEM = pltpu.MemorySpace.VMEM
SMEM = pltpu.MemorySpace.SMEM
f32 = jnp.float32
bf16 = jnp.bfloat16


def folded_ring(count):
    return list(range(0, count, 2)) + list(range(1, count, 2))[::-1]


def ring_step(value, ring):
    count = len(ring)
    return lax.ppermute(value, "sp", [(ring[i], ring[(i + 1) % count]) for i in range(count)])


def swap_groups(value):
    return lax.ppermute(value, "grp", [(0, 1), (1, 0)])


def gather_halves(half, ring):
    from_ring, from_group = [], []
    piece = half
    for _ in range(len(ring) - 1):
        piece = ring_step(piece, ring)
        from_ring.append(piece)
        from_group.append(swap_groups(piece))
    return from_ring, from_group


def exchange_columns(block, count):
    pieces = {0: block}
    step = count // 2
    while step:
        pairs = [(i, i ^ step) for i in range(count)]
        pieces.update({j ^ step: lax.ppermute(p, "tp", pairs) for j, p in list(pieces.items())})
        step //= 2
    return [pieces[j] for j in range(count)]


def full_spec(array):
    return pl.BlockSpec(array.shape, lambda i, n=array.ndim: (0,) * n)


def window_spec(shape, index):
    return pl.BlockSpec(shape, lambda i: index)


def call(kernel, order, operands, specs, out_shapes, scratch):
    return pl.pallas_call(
        kernel,
        grid=(1,),
        in_specs=[pl.BlockSpec(memory_space=SMEM)] + specs,
        out_specs=[pl.BlockSpec(o.shape, lambda i, n=len(o.shape): (0,) * n) for o in out_shapes],
        out_shape=out_shapes,
        scratch_shapes=scratch,
        compiler_params=pltpu.CompilerParams(vmem_limit_bytes=48 << 20),
    )(order, *operands)


def head_norm(raw, gain, head_size):
    parts = []
    for start in range(0, raw.shape[1], head_size):
        part = raw[:, start : start + head_size]
        parts.append(row_norm(part, gain))
    return jnp.concatenate(parts, axis=1)


def project(x_pieces, gain, q_gain, k_gain, own, pieces, piece_col, order, count):
    rows, piece_width = x_pieces[0].shape
    half = own[0].shape[0] // 2
    width = own[0].shape[1]
    dims = len(x_pieces) * piece_width
    blocks = dims // half
    per_piece = piece_width // half
    head_size = q_gain.shape[1]
    gain_blocks = gain.reshape(blocks, 1, half)
    operands = list(x_pieces) + [gain_blocks, q_gain, k_gain] + list(own)
    specs = [full_spec(a) for a in operands]
    for piece in pieces:
        for j in range(3):
            operands.append(piece)
            specs.append(window_spec((half, width), (0, piece_col + j)))
    n_x, n_p = len(x_pieces), len(pieces)

    def kernel(order_ref, *refs):
        x_refs, refs = refs[:n_x], refs[n_x:]
        gain_ref, qg_ref, kg_ref = refs[:3]
        own_refs, refs = refs[3:6], refs[6:]
        piece_refs, refs = refs[: 3 * n_p], refs[3 * n_p :]
        q_ref, kv_ref, xs = refs
        total = jnp.zeros((rows, 1), f32)
        for x_ref in x_refs:
            wide = x_ref[...].astype(f32)
            total = total + jnp.sum(wide * wide, axis=-1, keepdims=True)
        scale = lax.rsqrt(total / dims + epsilon)
        t = order_ref[count + 1]
        for j, x_ref in enumerate(x_refs):
            first = (t ^ j) * per_piece if n_x > 1 else 0
            for b in range(per_piece):
                wide = x_ref[:, b * half : (b + 1) * half].astype(f32)
                xs[first + b] = (wide * scale * gain_ref[first + b]).astype(bf16)
        grp = order_ref[count]
        sums = []
        for j in range(3):
            src = order_ref[0]
            acc = jnp.dot(xs[2 * src], own_refs[j][:half], preferred_element_type=f32)
            acc += jnp.dot(xs[2 * src + 1], own_refs[j][half:], preferred_element_type=f32)
            for k in range(n_p):
                src = order_ref[k // 2 + 1]
                part = grp if k % 2 == 0 else 1 - grp
                acc += jnp.dot(xs[2 * src + part], piece_refs[3 * k + j][...], preferred_element_type=f32)
            sums.append(acc)
        q_ref[...] = head_norm(sums[0], qg_ref[...], head_size).astype(bf16)
        kv_ref[:, :width] = head_norm(sums[1], kg_ref[...], head_size).astype(bf16)
        kv_ref[:, width:] = sums[2].astype(bf16)

    return call(
        kernel, order, operands, specs,
        [jax.ShapeDtypeStruct((rows, width), bf16), jax.ShapeDtypeStruct((rows, 2 * width), bf16)],
        [pltpu.VMEM((blocks, rows, half), bf16)],
    )


def attend_kernel(query, kv_parts, doc_col, doc_row, flat_bias, order, count, head_size):
    rows, width = query.shape
    reach = LEFT * SEG
    span = reach + rows
    depth = len(kv_parts) - 1
    extent = flat_bias.shape[-1]
    operands = [query] + list(kv_parts) + [doc_col, doc_row, flat_bias]
    specs = [full_spec(a) for a in operands]

    def kernel(order_ref, q_ref, *refs):
        kv_refs, refs = refs[: depth + 1], refs[depth + 1 :]
        dc_ref, dr_ref, fb_ref, out_ref = refs
        offset = order_ref[0] * rows
        seg_q = lax.broadcasted_iota(jnp.int32, (rows, span), 0) // SEG
        col = lax.broadcasted_iota(jnp.int32, (rows, span), 1)
        seg_k = col // SEG - LEFT
        allowed = (
            (seg_k <= seg_q) & (seg_k >= seg_q - LEFT) & (col >= reach - offset)
            & (dc_ref[...] == dr_ref[...])
        )
        outs = []
        for h in range(width // head_size):
            lo = h * head_size
            keys = jnp.concatenate([r[:, lo : lo + head_size] for r in kv_refs], axis=0)
            vals = jnp.concatenate([r[:, width + lo : width + lo + head_size] for r in kv_refs], axis=0)
            scores = lax.dot_general(
                q_ref[:, lo : lo + head_size], keys, (((1,), (1,)), ((), ())),
                preferred_element_type=f32,
            ) * head_size ** (-0.5)
            line = jnp.broadcast_to(fb_ref[h], (rows, extent))
            bias = pltpu.roll(line, 0, 1, stride=1, stride_axis=0)[:, :span]
            scores = jnp.where(allowed, scores + bias, -1e30)
            peak = jnp.max(scores, axis=-1, keepdims=True)
            expo = jnp.exp(scores - peak)
            weights = (expo / jnp.sum(expo, axis=-1, keepdims=True)).astype(bf16)
            outs.append(jnp.dot(weights, vals, preferred_element_type=f32))
        out_ref[...] = jnp.concatenate(outs, axis=1).astype(bf16)

    return call(kernel, order, operands, specs, [jax.ShapeDtypeStruct((rows, width), bf16)], [])[0]


def output(attended, residual, own, pieces, layer, order, count):
    rows, dims = attended.shape
    half = own.shape[0] // 2
    cols = own.shape[1]
    blocks = dims // half
    operands = [attended, residual, own] + list(pieces)
    specs = [full_spec(a) for a in operands[:3]]
    specs += [window_spec((half, cols), (layer, 0)) for _ in pieces]

    def kernel(order_ref, a_ref, r_ref, own_ref, *refs):
        piece_refs, (out_ref, xs) = refs[: len(pieces)], refs[len(pieces) :]
        for b in range(blocks):
            xs[b] = a_ref[:, b * half : (b + 1) * half]
        grp = order_ref[count]
        src = order_ref[0]
        acc = jnp.dot(xs[2 * src], own_ref[:half], preferred_element_type=f32)
        acc += jnp.dot(xs[2 * src + 1], own_ref[half:], preferred_element_type=f32)
        for k in range(len(pieces)):
            src = order_ref[k // 2 + 1]
            part = grp if k % 2 == 0 else 1 - grp
            acc += jnp.dot(xs[2 * src + part], piece_refs[k][...], preferred_element_type=f32)
        out_ref[...] = (r_ref[...].astype(f32) + acc).astype(bf16)

    return call(
        kernel, order, operands, specs, [jax.ShapeDtypeStruct((rows, cols), bf16)],
        [pltpu.VMEM((blocks, rows, half), bf16)],
    )[0]


def assemble(pieces, order, count):
    rows, cols = pieces[0].shape

    def kernel(order_ref, *refs):
        t = order_ref[count + 1]
        for j in range(len(pieces)):
            start = pl.multiple_of((t ^ j) * cols, cols)
            refs[-1][:, pl.ds(start, cols)] = refs[j][...]

    return call(
        kernel, order, pieces, [full_spec(a) for a in pieces],
        [jax.ShapeDtypeStruct((rows, cols * len(pieces)), bf16)], [],
    )[0]


def flat_biases(rel_bias, rows):
    reach = LEFT * SEG
    heads_here = rel_bias.shape[0]
    extent = 128 * (-(-(reach + 2 * rows - 1) // 128))
    far = jnp.broadcast_to(rel_bias[:, -1:], (heads_here, reach - MAXREL))
    near = rel_bias[:, MAXREL - rows + 1 :][:, ::-1]
    tail = jnp.broadcast_to(rel_bias[:, -1:], (heads_here, extent - reach - rows))
    return jnp.concatenate([far, near, tail], axis=1)[:, None, :]


def interleave(ring_pieces, group_pieces):
    return [p for pair in zip(ring_pieces, group_pieces) for p in pair]


def on_device_fast(
    stream, doc_ids, norm_gain, query_weight, key_weight, value_weight, out_weight,
    query_gain, key_gain, rel_bias,
):
    rows = stream.shape[0]
    count = lax.axis_size("sp")
    tp_count = lax.axis_size("tp")
    grp = lax.axis_index("grp")
    place = lax.axis_index("sp")
    t = lax.axis_index("tp")
    head_size = query_gain.shape[1]
    reach = LEFT * SEG
    depth = -(-reach // rows)
    cols = out_weight.shape[2]
    ring = folded_ring(count)
    slots = jnp.array([ring.index(i) for i in range(count)], jnp.int32)
    ring_of = jnp.array(ring, jnp.int32)
    steps = jnp.arange(count, dtype=jnp.int32)
    sources = ring_of[(slots[place] - steps) % count]
    order = jnp.concatenate([sources, jnp.stack([grp, t]).astype(jnp.int32)])

    in_half = query_weight.shape[1] // 2
    out_half = out_weight.shape[1] // 2

    def half_of(weight, size):
        return lax.dynamic_slice_in_dim(weight, grp * size, size, 0)

    first = jnp.concatenate(
        [half_of(w[0], in_half) for w in (query_weight, key_weight, value_weight)], axis=1
    )
    outs = jnp.concatenate([half_of(out_weight[l], out_half) for l in range(LAYERS)], axis=0)
    second = jnp.concatenate(
        [outs] + [half_of(w[1], in_half) for w in (query_weight, key_weight, value_weight)], axis=1
    )
    a_ring, a_group = gather_halves(first, ring)
    second, _ = lax.optimization_barrier((second, a_ring[-1]))
    b_ring, b_group = gather_halves(second, ring)
    a_pieces = interleave(a_ring, a_group)
    b_pieces = interleave(b_ring, b_group)

    all_docs = lax.all_gather(doc_ids, "sp", axis=0, tiled=True)
    padded = jnp.concatenate([jnp.full((reach,), -1, jnp.int32), all_docs])
    doc_row = lax.dynamic_slice_in_dim(padded, place * rows, reach + rows, 0)[None, :]
    doc_col = doc_ids[:, None]
    flat = flat_biases(rel_bias, rows)

    residual = lax.dynamic_slice_in_dim(stream, t * cols, cols, 1)
    x_pieces = [stream]
    for layer in range(LAYERS):
        own = [w[layer] for w in (query_weight, key_weight, value_weight)]
        pieces = a_pieces if layer == 0 else b_pieces
        col = 0 if layer == 0 else cols // own[0].shape[1]
        query, kv = project(
            x_pieces, norm_gain[layer], query_gain[layer][None], key_gain[layer][None],
            own, pieces, col, order, count,
        )
        received = [shifted(kv, "sp", back) for back in range(depth, 0, -1)]
        attended = attend_kernel(
            query, received + [kv], doc_col, doc_row, flat, order, count, head_size
        )
        all_heads = lax.all_gather(attended, "tp", axis=1, tiled=True)
        block = output(all_heads, residual, out_weight[layer], b_pieces, layer, order, count)
        x_pieces = exchange_columns(block, tp_count)
        residual = block
    return assemble(x_pieces, order, count)


def on_device(*arrays):
    stream, query_weight, out_weight = arrays[0], arrays[3], arrays[6]
    rows, dims = stream.shape
    count, tp_count = lax.axis_size("sp"), lax.axis_size("tp")
    in_rows, width = query_weight.shape[1:]
    out_rows, cols = out_weight.shape[1:]
    fits = (
        lax.axis_size("grp") == 2 and LAYERS == 2
        and 2 < count <= 4 and tp_count & (tp_count - 1) == 0
        and in_rows % 256 == 0 and out_rows % 256 == 0
        and 2 * (out_rows // 2) == in_rows // 2
        and width % 128 == 0 and cols % width == 0
        and cols % (in_rows // 2) == 0 and tp_count > 1
        and rows <= MAXREL and (LEFT * SEG) % rows == 0 and rows % SEG == 0
    )
    return on_device_fast(*arrays) if fits else on_device_general(*arrays)


def solution(mesh):
    placed = (
        P(("grp", "sp"), None),
        P(("grp", "sp")),
        P(),
        P(None, "sp", "tp"),
        P(None, "sp", "tp"),
        P(None, "sp", "tp"),
        P(None, "sp", "tp"),
        P(),
        P(),
        P("tp", None),
    )
    return jax.shard_map(
        on_device, mesh=mesh, in_specs=placed, out_specs=P(("grp", "sp"), None), check_vma=False
    )
```

```python
import jax
import jax.numpy as jnp
from jax import lax
from jax.experimental import pallas as pl
from jax.experimental.pallas import tpu as pltpu
from jax.sharding import PartitionSpec as P

SEG = 64
LEFT = 8
MAXREL = 256
LAYERS = 2


epsilon = 1e-06


def shifted(value, axis, steps):
    count = lax.axis_size(axis)
    initial, last = (max(0, -steps), min(count, count - steps))
    return lax.ppermute(value, axis, [(source, source + steps) for source in range(initial, last)])


def row_norm(values, gain):
    return values * lax.rsqrt(jnp.mean(values * values, axis=-1, keepdims=True) + epsilon) * gain


def bias_table(rel_bias):
    heads_here = rel_bias.shape[0]
    reach = LEFT * SEG
    width = (LEFT + 1) * SEG
    highest = reach + SEG - 1
    reversed_bias = rel_bias[:, ::-1]
    upper_fill = jnp.broadcast_to(rel_bias[:, -1:], (heads_here, highest - MAXREL))
    flat_row = jnp.concatenate([upper_fill, reversed_bias[:, : MAXREL + SEG]], axis=1)
    lines = [
        flat_row[:, SEG - 1 - position : SEG - 1 - position + width] for position in range(SEG)
    ]
    return jnp.stack(lines, axis=1)


def attend(query, ext_keys, ext_values, ext_docs, own_docs, offset, table):
    rows, heads_here, head_size = query.shape
    count = rows // SEG
    width = (LEFT + 1) * SEG
    blocks = query.reshape(count, SEG, heads_here, head_size)
    key_blocks = ext_keys.reshape(count + LEFT, SEG, heads_here, head_size)
    value_blocks = ext_values.reshape(count + LEFT, SEG, heads_here, head_size)
    doc_blocks = ext_docs.reshape(count + LEFT, SEG)
    score_parts = [
        jnp.einsum(
            "nqhd,nkhd->nhqk",
            blocks,
            key_blocks[earlier : earlier + count],
            preferred_element_type=jnp.float32,
        )
        for earlier in range(LEFT + 1)
    ]
    scores = jnp.concatenate(score_parts, axis=-1)
    scores = scores * head_size ** (-0.5) + table[None]
    doc_band = jnp.concatenate(
        [doc_blocks[earlier : earlier + count] for earlier in range(LEFT + 1)], axis=1
    )
    key_pos = (
        offset
        + SEG * jnp.arange(count, dtype=jnp.int32)[:, None]
        - LEFT * SEG
        + jnp.arange(width, dtype=jnp.int32)[None, :]
    )
    allowed = (key_pos >= 0)[:, None, None, :] & (
        doc_band[:, None, None, :] == own_docs.reshape(count, SEG)[:, None, :, None]
    )
    scores = jnp.where(allowed, scores, -1e30)
    peak = jnp.max(scores, axis=-1, keepdims=True)
    expo = jnp.exp(scores - peak)
    weights = (expo / jnp.sum(expo, axis=-1, keepdims=True)).astype(jnp.bfloat16)
    mixed = jnp.zeros((count, SEG, heads_here, head_size), jnp.float32)
    for earlier in range(LEFT + 1):
        part_weights = weights[..., earlier * SEG : (earlier + 1) * SEG]
        mixed = mixed + jnp.einsum(
            "nhqk,nkhd->nqhd",
            part_weights,
            value_blocks[earlier : earlier + count],
            preferred_element_type=jnp.float32,
        )
    return mixed.astype(jnp.bfloat16).reshape(rows, heads_here * head_size)


def on_device_general(
    stream,
    doc_ids,
    norm_gain,
    query_weight,
    key_weight,
    value_weight,
    out_weight,
    query_gain,
    key_gain,
    rel_bias,
):
    rows = stream.shape[0]
    heads_here = rel_bias.shape[0]
    head_size = query_gain.shape[1]
    local_width = heads_here * head_size
    reach = LEFT * SEG
    depth = -(-reach // rows)
    offset = lax.axis_index("sp") * rows
    col_width = out_weight.shape[2]
    col_start = lax.axis_index("tp") * col_width
    table = bias_table(rel_bias)
    x = stream
    for layer in range(LAYERS):
        widened = x.astype(jnp.float32)
        normed = row_norm(widened, norm_gain[layer]).astype(jnp.bfloat16)
        own_cols = normed
        q_raw = jnp.dot(
            own_cols,
            lax.all_gather(query_weight[layer], "sp", axis=0, tiled=True),
            preferred_element_type=jnp.float32,
        )
        k_raw = jnp.dot(
            normed,
            lax.all_gather(key_weight[layer], "sp", axis=0, tiled=True),
            preferred_element_type=jnp.float32,
        )
        v_raw = jnp.dot(
            normed,
            lax.all_gather(value_weight[layer], "sp", axis=0, tiled=True),
            preferred_element_type=jnp.float32,
        )
        query = row_norm(q_raw.reshape(rows, heads_here, head_size), query_gain[layer]).astype(
            jnp.bfloat16
        )
        keys = row_norm(
            k_raw.reshape(normed.shape[0], heads_here, head_size), key_gain[layer]
        ).astype(jnp.bfloat16)
        values = v_raw.astype(jnp.bfloat16)
        flat_keys = keys.reshape(rows, local_width)
        tail = (flat_keys, values, doc_ids)
        received = [
            shifted((tail[0], tail[1], tail[2]), "sp", distance_back)
            for distance_back in range(depth, 0, -1)
        ]
        ext_keys = jnp.concatenate([item[0] for item in received] + [flat_keys], axis=0)
        ext_values = jnp.concatenate([item[1] for item in received] + [values], axis=0)
        ext_docs = jnp.concatenate([item[2] for item in received] + [doc_ids], axis=0)
        ext_keys = ext_keys.reshape(reach + rows, heads_here, head_size)
        ext_values = ext_values.reshape(reach + rows, heads_here, head_size)
        attended = attend(query, ext_keys, ext_values, ext_docs, doc_ids, offset, table)
        all_heads = lax.all_gather(attended, "tp", axis=1, tiled=True)
        projected = jnp.dot(
            all_heads,
            lax.all_gather(out_weight[layer], "sp", axis=0, tiled=True),
            preferred_element_type=jnp.float32,
        )
        own_cols = lax.dynamic_slice_in_dim(widened, col_start, col_width, 1)
        new_cols = (own_cols + projected).astype(jnp.bfloat16)
        x = lax.all_gather(new_cols, "tp", axis=1, tiled=True)
    return x


VMEM = pltpu.MemorySpace.VMEM
SMEM = pltpu.MemorySpace.SMEM
f32 = jnp.float32
bf16 = jnp.bfloat16


def folded_ring(count):
    return list(range(0, count, 2)) + list(range(1, count, 2))[::-1]


def ring_step(value, ring):
    count = len(ring)
    return lax.ppermute(value, "sp", [(ring[i], ring[(i + 1) % count]) for i in range(count)])


def tie(value, *others):
    return lax.optimization_barrier((value,) + others)[0]


def swap_groups(value):
    return lax.ppermute(value, "grp", [(0, 1), (1, 0)])


def exchange_columns(block, count):
    pieces = {0: block}
    step = count // 2
    while step:
        pairs = [(i, i ^ step) for i in range(count)]
        pieces.update({j ^ step: lax.ppermute(p, "tp", pairs) for j, p in list(pieces.items())})
        step //= 2
    return [pieces[j] for j in range(count)]


def full_spec(array):
    return pl.BlockSpec(array.shape, lambda i, n=array.ndim: (0,) * n)


def window_spec(shape, index):
    return pl.BlockSpec(shape, lambda i: index)


def call(kernel, order, operands, specs, out_shapes, scratch):
    return pl.pallas_call(
        kernel,
        grid=(1,),
        in_specs=[pl.BlockSpec(memory_space=SMEM)] + specs,
        out_specs=[pl.BlockSpec(o.shape, lambda i, n=len(o.shape): (0,) * n) for o in out_shapes],
        out_shape=out_shapes,
        scratch_shapes=scratch,
        compiler_params=pltpu.CompilerParams(vmem_limit_bytes=48 << 20),
    )(order, *operands)


def head_norm(raw, gain, head_size):
    parts = []
    for start in range(0, raw.shape[1], head_size):
        part = raw[:, start : start + head_size]
        parts.append(row_norm(part, gain))
    return jnp.concatenate(parts, axis=1)


def project(x_pieces, gain, q_gain, k_gain, own, pieces, piece_col, order, count):
    rows, piece_width = x_pieces[0].shape
    half = own[0].shape[0] // 2
    width = own[0].shape[1]
    dims = len(x_pieces) * piece_width
    blocks = dims // half
    per_piece = piece_width // half
    head_size = q_gain.shape[1]
    gain_blocks = gain.reshape(blocks, 1, half)
    operands = list(x_pieces) + [gain_blocks, q_gain, k_gain] + list(own)
    specs = [full_spec(a) for a in operands]
    for piece in pieces:
        for j in range(3):
            operands.append(piece)
            specs.append(window_spec((half, width), (0, piece_col + j)))
    n_x, n_p = len(x_pieces), len(pieces)

    def kernel(order_ref, *refs):
        x_refs, refs = refs[:n_x], refs[n_x:]
        gain_ref, qg_ref, kg_ref = refs[:3]
        own_refs, refs = refs[3:6], refs[6:]
        piece_refs, refs = refs[: 3 * n_p], refs[3 * n_p :]
        q_ref, kv_ref, xs = refs
        total = jnp.zeros((rows, 1), f32)
        for x_ref in x_refs:
            wide = x_ref[...].astype(f32)
            total = total + jnp.sum(wide * wide, axis=-1, keepdims=True)
        scale = lax.rsqrt(total / dims + epsilon)
        t = order_ref[count + 1]
        for j, x_ref in enumerate(x_refs):
            first = (t ^ j) * per_piece if n_x > 1 else 0
            for b in range(per_piece):
                wide = x_ref[:, b * half : (b + 1) * half].astype(f32)
                xs[first + b] = (wide * scale * gain_ref[first + b]).astype(bf16)
        grp = order_ref[count]
        sums = []
        for j in range(3):
            src = order_ref[0]
            acc = jnp.dot(xs[2 * src], own_refs[j][:half], preferred_element_type=f32)
            acc += jnp.dot(xs[2 * src + 1], own_refs[j][half:], preferred_element_type=f32)
            for k in range(n_p):
                src = order_ref[k // 2 + 1]
                part = grp if k % 2 == 0 else 1 - grp
                acc += jnp.dot(xs[2 * src + part], piece_refs[3 * k + j][...], preferred_element_type=f32)
            sums.append(acc)
        q_ref[...] = head_norm(sums[0], qg_ref[...], head_size).astype(bf16)
        kv_ref[:, :width] = head_norm(sums[1], kg_ref[...], head_size).astype(bf16)
        kv_ref[:, width:] = sums[2].astype(bf16)

    return call(
        kernel, order, operands, specs,
        [jax.ShapeDtypeStruct((rows, width), bf16), jax.ShapeDtypeStruct((rows, 2 * width), bf16)],
        [pltpu.VMEM((blocks, rows, half), bf16)],
    )


def attend_kernel(query, kv_parts, doc_col, doc_row, flat_bias, order, count, head_size):
    rows, width = query.shape
    reach = LEFT * SEG
    span = reach + rows
    depth = len(kv_parts) - 1
    extent = flat_bias.shape[-1]
    operands = [query] + list(kv_parts) + [doc_col, doc_row, flat_bias]
    specs = [full_spec(a) for a in operands]

    def kernel(order_ref, q_ref, *refs):
        kv_refs, refs = refs[: depth + 1], refs[depth + 1 :]
        dc_ref, dr_ref, fb_ref, out_ref = refs
        offset = order_ref[0] * rows
        seg_q = lax.broadcasted_iota(jnp.int32, (rows, span), 0) // SEG
        col = lax.broadcasted_iota(jnp.int32, (rows, span), 1)
        seg_k = col // SEG - LEFT
        allowed = (
            (seg_k <= seg_q) & (seg_k >= seg_q - LEFT) & (col >= reach - offset)
            & (dc_ref[...] == dr_ref[...])
        )
        outs = []
        for h in range(width // head_size):
            lo = h * head_size
            keys = jnp.concatenate([r[:, lo : lo + head_size] for r in kv_refs], axis=0)
            vals = jnp.concatenate([r[:, width + lo : width + lo + head_size] for r in kv_refs], axis=0)
            scores = lax.dot_general(
                q_ref[:, lo : lo + head_size], keys, (((1,), (1,)), ((), ())),
                preferred_element_type=f32,
            ) * head_size ** (-0.5)
            line = jnp.broadcast_to(fb_ref[h], (rows, extent))
            bias = pltpu.roll(line, 0, 1, stride=1, stride_axis=0)[:, :span]
            scores = jnp.where(allowed, scores + bias, -1e30)
            peak = jnp.max(scores, axis=-1, keepdims=True)
            expo = jnp.exp(scores - peak)
            weights = (expo / jnp.sum(expo, axis=-1, keepdims=True)).astype(bf16)
            outs.append(jnp.dot(weights, vals, preferred_element_type=f32))
        out_ref[...] = jnp.concatenate(outs, axis=1).astype(bf16)

    return call(kernel, order, operands, specs, [jax.ShapeDtypeStruct((rows, width), bf16)], [])[0]


def output(attended, residual, own, pieces, order, count):
    rows, dims = attended.shape
    half = own.shape[0] // 2
    cols = own.shape[1]
    blocks = dims // half
    operands = [attended, residual, own] + list(pieces)
    specs = [full_spec(a) for a in operands[:3]]
    packed = pieces[0].shape[0] != half
    shape = (2 * half, cols // 2) if packed else (half, cols)
    specs += [window_spec(shape, (0, 0)) for _ in pieces]

    def kernel(order_ref, a_ref, r_ref, own_ref, *refs):
        piece_refs, (out_ref, xs) = refs[: len(pieces)], refs[len(pieces) :]
        for b in range(blocks):
            xs[b] = a_ref[:, b * half : (b + 1) * half]
        grp = order_ref[count]
        src = order_ref[0]
        acc = jnp.dot(xs[2 * src], own_ref[:half], preferred_element_type=f32)
        acc += jnp.dot(xs[2 * src + 1], own_ref[half:], preferred_element_type=f32)
        for k in range(len(pieces)):
            src = order_ref[k // 2 + 1]
            part = grp if k % 2 == 0 else 1 - grp
            weight = piece_refs[k][...]
            if packed:
                weight = jnp.concatenate([weight[:half], weight[half:]], axis=1)
            acc += jnp.dot(xs[2 * src + part], weight, preferred_element_type=f32)
        out_ref[...] = (r_ref[...].astype(f32) + acc).astype(bf16)

    return call(
        kernel, order, operands, specs, [jax.ShapeDtypeStruct((rows, cols), bf16)],
        [pltpu.VMEM((blocks, rows, half), bf16)],
    )[0]


def assemble(pieces, order, count):
    rows, cols = pieces[0].shape

    def kernel(order_ref, *refs):
        t = order_ref[count + 1]
        for j in range(len(pieces)):
            start = pl.multiple_of((t ^ j) * cols, cols)
            refs[-1][:, pl.ds(start, cols)] = refs[j][...]

    return call(
        kernel, order, pieces, [full_spec(a) for a in pieces],
        [jax.ShapeDtypeStruct((rows, cols * len(pieces)), bf16)], [],
    )[0]


def flat_biases(rel_bias, rows):
    reach = LEFT * SEG
    heads_here = rel_bias.shape[0]
    extent = 128 * (-(-(reach + 2 * rows - 1) // 128))
    far = jnp.broadcast_to(rel_bias[:, -1:], (heads_here, reach - MAXREL))
    near = rel_bias[:, MAXREL - rows + 1 :][:, ::-1]
    tail = jnp.broadcast_to(rel_bias[:, -1:], (heads_here, extent - reach - rows))
    return jnp.concatenate([far, near, tail], axis=1)[:, None, :]


def interleave(ring_pieces, group_pieces):
    return [p for pair in zip(ring_pieces, group_pieces) for p in pair]


def on_device_fast(
    stream, doc_ids, norm_gain, query_weight, key_weight, value_weight, out_weight,
    query_gain, key_gain, rel_bias,
):
    rows = stream.shape[0]
    count = lax.axis_size("sp")
    tp_count = lax.axis_size("tp")
    grp = lax.axis_index("grp")
    place = lax.axis_index("sp")
    t = lax.axis_index("tp")
    head_size = query_gain.shape[1]
    reach = LEFT * SEG
    depth = -(-reach // rows)
    cols = out_weight.shape[2]
    ring = folded_ring(count)
    slots = jnp.array([ring.index(i) for i in range(count)], jnp.int32)
    ring_of = jnp.array(ring, jnp.int32)
    steps = jnp.arange(count, dtype=jnp.int32)
    sources = ring_of[(slots[place] - steps) % count]
    order = jnp.concatenate([sources, jnp.stack([grp, t]).astype(jnp.int32)])

    in_half = query_weight.shape[1] // 2
    out_half = out_weight.shape[1] // 2

    def half_of(weight, size):
        return lax.dynamic_slice_in_dim(weight, grp * size, size, 0)

    def joined(layer):
        shards = (query_weight, key_weight, value_weight)
        return jnp.concatenate([half_of(w[layer], in_half) for w in shards], axis=1)

    first = joined(0)
    out_first = half_of(out_weight[0], out_half)
    a_ring, a_group = [ring_step(first, ring)], []
    own_next = half_of(out_weight[1], out_half)
    own_next = jnp.concatenate([own_next[:, : cols // 2], own_next[:, cols // 2 :]], axis=0)
    second = jnp.concatenate([own_next, joined(1)], axis=1)
    second = tie(second, a_ring[0])
    docs = [tie(doc_ids, a_ring[0])]
    docs = [shifted(docs[0], "sp", back) for back in range(depth, 0, -1)] + docs
    for step in range(1, count - 1):
        source = tie(a_ring[-1], *a_group[-1:], *(docs if step > 1 else [second]))
        a_group.append(swap_groups(a_ring[-1]))
        a_ring.append(ring_step(source, ring))
    last, base = a_ring[-1], a_group[-1]
    a_group.append(swap_groups(tie(last, base)))
    c_ring, c_group = [ring_step(tie(second, last, base), ring)], []
    doc_row = jnp.concatenate(docs)[None, :]
    doc_col = doc_ids[:, None]
    flat = flat_biases(rel_bias, rows)

    residual = tie(lax.dynamic_slice_in_dim(stream, t * cols, cols, 1), a_ring[0])
    x_pieces = [stream]
    piece_cols = own_next.shape[1]
    for layer in range(LAYERS):
        own = [w[layer] for w in (query_weight, key_weight, value_weight)]
        ring_pieces, group_pieces = (a_ring, a_group) if layer == 0 else (c_ring, c_group)
        col = 0 if layer == 0 else piece_cols // own[0].shape[1]
        query, kv = project(
            x_pieces, norm_gain[layer], query_gain[layer][None], key_gain[layer][None],
            own, interleave(ring_pieces, group_pieces), col,
            tie(order, c_ring[0]) if layer == 0 else order, count,
        )
        received = [shifted(kv, "sp", back) for back in range(depth, 0, -1)]
        attend_order = out_order = order
        if layer == 0:
            o_ring, o_group = [ring_step(tie(out_first, kv), ring)], []
            c_group.append(swap_groups(tie(c_ring[0], kv)))
            for step in range(1, count - 1):
                near = received[-1] if step == 1 else o_group[-1]
                o_group.append(swap_groups(tie(o_ring[-1], near)))
                o_ring.append(ring_step(tie(o_ring[-1], near), ring))
            attend_order = tie(order, o_ring[-1], o_group[-1], c_group[-1])
            o_group.append(swap_groups(tie(o_ring[-1], attend_order)))
            c_ring.append(ring_step(tie(c_ring[0], received[0], attend_order), ring))
        attended = attend_kernel(
            query, received + [kv], doc_col, doc_row, flat, attend_order, count, head_size
        )
        all_heads = lax.all_gather(attended, "tp", axis=1, tiled=True)
        if layer == 0:
            out_order = tie(order, c_ring[-1])
            for step in range(2, count - 1):
                c_group.append(swap_groups(tie(c_ring[-1], all_heads)))
                c_ring.append(ring_step(tie(c_ring[-1], all_heads), ring))
            o_pieces = interleave(o_ring, o_group)
        else:
            o_pieces = interleave(c_ring, c_group)
        block = output(all_heads, residual, out_weight[layer], o_pieces, out_order, count)
        x_pieces = exchange_columns(block, tp_count)
        if layer == 0:
            c_group.append(swap_groups(c_ring[-1]))
        residual = block
    return assemble(x_pieces, order, count)


def on_device(*arrays):
    stream, query_weight, out_weight = arrays[0], arrays[3], arrays[6]
    rows, dims = stream.shape
    count, tp_count = lax.axis_size("sp"), lax.axis_size("tp")
    in_rows, width = query_weight.shape[1:]
    out_rows, cols = out_weight.shape[1:]
    fits = (
        lax.axis_size("grp") == 2 and LAYERS == 2
        and count == 4 and tp_count & (tp_count - 1) == 0
        and in_rows % 256 == 0 and out_rows % 256 == 0
        and 2 * (out_rows // 2) == in_rows // 2
        and width % 128 == 0 and cols % (2 * width) == 0
        and cols % (in_rows // 2) == 0 and tp_count > 1
        and rows <= MAXREL and (LEFT * SEG) % rows == 0 and rows % SEG == 0
    )
    return on_device_fast(*arrays) if fits else on_device_general(*arrays)


def solution(mesh):
    placed = (
        P(("grp", "sp"), None),
        P(("grp", "sp")),
        P(),
        P(None, "sp", "tp"),
        P(None, "sp", "tp"),
        P(None, "sp", "tp"),
        P(None, "sp", "tp"),
        P(),
        P(),
        P("tp", None),
    )
    return jax.shard_map(
        on_device, mesh=mesh, in_specs=placed, out_specs=P(("grp", "sp"), None), check_vma=False
    )
```

```python
import jax
import jax.numpy as jnp
from jax import lax
from jax.experimental import pallas as pl
from jax.experimental.pallas import tpu as pltpu
from jax.sharding import PartitionSpec as P

SEG = 64
LEFT = 8
MAXREL = 256
LAYERS = 2


epsilon = 1e-06


def shifted(value, axis, steps):
    count = lax.axis_size(axis)
    initial, last = (max(0, -steps), min(count, count - steps))
    return lax.ppermute(value, axis, [(source, source + steps) for source in range(initial, last)])


def row_norm(values, gain):
    return values * lax.rsqrt(jnp.mean(values * values, axis=-1, keepdims=True) + epsilon) * gain


def bias_table(rel_bias):
    heads_here = rel_bias.shape[0]
    reach = LEFT * SEG
    width = (LEFT + 1) * SEG
    highest = reach + SEG - 1
    reversed_bias = rel_bias[:, ::-1]
    upper_fill = jnp.broadcast_to(rel_bias[:, -1:], (heads_here, highest - MAXREL))
    flat_row = jnp.concatenate([upper_fill, reversed_bias[:, : MAXREL + SEG]], axis=1)
    lines = [
        flat_row[:, SEG - 1 - position : SEG - 1 - position + width] for position in range(SEG)
    ]
    return jnp.stack(lines, axis=1)


def attend(query, ext_keys, ext_values, ext_docs, own_docs, offset, table):
    rows, heads_here, head_size = query.shape
    count = rows // SEG
    width = (LEFT + 1) * SEG
    blocks = query.reshape(count, SEG, heads_here, head_size)
    key_blocks = ext_keys.reshape(count + LEFT, SEG, heads_here, head_size)
    value_blocks = ext_values.reshape(count + LEFT, SEG, heads_here, head_size)
    doc_blocks = ext_docs.reshape(count + LEFT, SEG)
    score_parts = [
        jnp.einsum(
            "nqhd,nkhd->nhqk",
            blocks,
            key_blocks[earlier : earlier + count],
            preferred_element_type=jnp.float32,
        )
        for earlier in range(LEFT + 1)
    ]
    scores = jnp.concatenate(score_parts, axis=-1)
    scores = scores * head_size ** (-0.5) + table[None]
    doc_band = jnp.concatenate(
        [doc_blocks[earlier : earlier + count] for earlier in range(LEFT + 1)], axis=1
    )
    key_pos = (
        offset
        + SEG * jnp.arange(count, dtype=jnp.int32)[:, None]
        - LEFT * SEG
        + jnp.arange(width, dtype=jnp.int32)[None, :]
    )
    allowed = (key_pos >= 0)[:, None, None, :] & (
        doc_band[:, None, None, :] == own_docs.reshape(count, SEG)[:, None, :, None]
    )
    scores = jnp.where(allowed, scores, -1e30)
    peak = jnp.max(scores, axis=-1, keepdims=True)
    expo = jnp.exp(scores - peak)
    weights = (expo / jnp.sum(expo, axis=-1, keepdims=True)).astype(jnp.bfloat16)
    mixed = jnp.zeros((count, SEG, heads_here, head_size), jnp.float32)
    for earlier in range(LEFT + 1):
        part_weights = weights[..., earlier * SEG : (earlier + 1) * SEG]
        mixed = mixed + jnp.einsum(
            "nhqk,nkhd->nqhd",
            part_weights,
            value_blocks[earlier : earlier + count],
            preferred_element_type=jnp.float32,
        )
    return mixed.astype(jnp.bfloat16).reshape(rows, heads_here * head_size)


def on_device_general(
    stream,
    doc_ids,
    norm_gain,
    query_weight,
    key_weight,
    value_weight,
    out_weight,
    query_gain,
    key_gain,
    rel_bias,
):
    rows = stream.shape[0]
    heads_here = rel_bias.shape[0]
    head_size = query_gain.shape[1]
    local_width = heads_here * head_size
    reach = LEFT * SEG
    depth = -(-reach // rows)
    offset = lax.axis_index("sp") * rows
    col_width = out_weight.shape[2]
    col_start = lax.axis_index("tp") * col_width
    table = bias_table(rel_bias)
    x = stream
    for layer in range(LAYERS):
        widened = x.astype(jnp.float32)
        normed = row_norm(widened, norm_gain[layer]).astype(jnp.bfloat16)
        own_cols = normed
        q_raw = jnp.dot(
            own_cols,
            lax.all_gather(query_weight[layer], "sp", axis=0, tiled=True),
            preferred_element_type=jnp.float32,
        )
        k_raw = jnp.dot(
            normed,
            lax.all_gather(key_weight[layer], "sp", axis=0, tiled=True),
            preferred_element_type=jnp.float32,
        )
        v_raw = jnp.dot(
            normed,
            lax.all_gather(value_weight[layer], "sp", axis=0, tiled=True),
            preferred_element_type=jnp.float32,
        )
        query = row_norm(q_raw.reshape(rows, heads_here, head_size), query_gain[layer]).astype(
            jnp.bfloat16
        )
        keys = row_norm(
            k_raw.reshape(normed.shape[0], heads_here, head_size), key_gain[layer]
        ).astype(jnp.bfloat16)
        values = v_raw.astype(jnp.bfloat16)
        flat_keys = keys.reshape(rows, local_width)
        tail = (flat_keys, values, doc_ids)
        received = [
            shifted((tail[0], tail[1], tail[2]), "sp", distance_back)
            for distance_back in range(depth, 0, -1)
        ]
        ext_keys = jnp.concatenate([item[0] for item in received] + [flat_keys], axis=0)
        ext_values = jnp.concatenate([item[1] for item in received] + [values], axis=0)
        ext_docs = jnp.concatenate([item[2] for item in received] + [doc_ids], axis=0)
        ext_keys = ext_keys.reshape(reach + rows, heads_here, head_size)
        ext_values = ext_values.reshape(reach + rows, heads_here, head_size)
        attended = attend(query, ext_keys, ext_values, ext_docs, doc_ids, offset, table)
        all_heads = lax.all_gather(attended, "tp", axis=1, tiled=True)
        projected = jnp.dot(
            all_heads,
            lax.all_gather(out_weight[layer], "sp", axis=0, tiled=True),
            preferred_element_type=jnp.float32,
        )
        own_cols = lax.dynamic_slice_in_dim(widened, col_start, col_width, 1)
        new_cols = (own_cols + projected).astype(jnp.bfloat16)
        x = lax.all_gather(new_cols, "tp", axis=1, tiled=True)
    return x


VMEM = pltpu.MemorySpace.VMEM
SMEM = pltpu.MemorySpace.SMEM
f32 = jnp.float32
bf16 = jnp.bfloat16


def folded_ring(count):
    return list(range(0, count, 2)) + list(range(1, count, 2))[::-1]


def ring_step(value, ring):
    count = len(ring)
    return lax.ppermute(value, "sp", [(ring[i], ring[(i + 1) % count]) for i in range(count)])


def tie(value, *others):
    return lax.optimization_barrier((value,) + others)[0]


def swap_groups(value):
    return lax.ppermute(value, "grp", [(0, 1), (1, 0)])


def exchange_columns(block, count):
    pieces = {0: block}
    step = count // 2
    while step:
        pairs = [(i, i ^ step) for i in range(count)]
        pieces.update({j ^ step: lax.ppermute(p, "tp", pairs) for j, p in list(pieces.items())})
        step //= 2
    return [pieces[j] for j in range(count)]


def full_spec(array):
    return pl.BlockSpec(array.shape, lambda i, n=array.ndim: (0,) * n)


def window_spec(shape, index):
    return pl.BlockSpec(shape, lambda i: index)


def call(kernel, order, operands, specs, out_shapes, scratch):
    return pl.pallas_call(
        kernel,
        grid=(1,),
        in_specs=[pl.BlockSpec(memory_space=SMEM)] + specs,
        out_specs=[pl.BlockSpec(o.shape, lambda i, n=len(o.shape): (0,) * n) for o in out_shapes],
        out_shape=out_shapes,
        scratch_shapes=scratch,
        compiler_params=pltpu.CompilerParams(vmem_limit_bytes=48 << 20),
    )(order, *operands)


def head_norm(raw, gain, head_size):
    parts = []
    for start in range(0, raw.shape[1], head_size):
        part = raw[:, start : start + head_size]
        parts.append(row_norm(part, gain))
    return jnp.concatenate(parts, axis=1)


def project(x_pieces, gain, q_gain, k_gain, own, layer, pieces, order, count):
    rows, piece_width = x_pieces[0].shape
    half = own[0].shape[1] // 2
    width = own[0].shape[2]
    dims = len(x_pieces) * piece_width
    blocks = dims // half
    per_piece = piece_width // half
    head_size = q_gain.shape[1]
    gain_blocks = gain.reshape(blocks, 1, half)
    operands = list(x_pieces) + [gain_blocks, q_gain, k_gain]
    specs = [full_spec(a) for a in operands]
    operands += list(own)
    specs += [window_spec((1, 2 * half, width), (layer, 0, 0)) for _ in own]
    for piece in pieces:
        for j in range(3):
            operands.append(piece)
            specs.append(window_spec((half, width), (0, j)))
    n_x, n_p = len(x_pieces), len(pieces)

    def kernel(order_ref, *refs):
        x_refs, refs = refs[:n_x], refs[n_x:]
        gain_ref, qg_ref, kg_ref = refs[:3]
        own_refs, refs = refs[3:6], refs[6:]
        piece_refs, refs = refs[: 3 * n_p], refs[3 * n_p :]
        q_ref, kv_ref, xs = refs
        total = jnp.zeros((rows, 1), f32)
        for x_ref in x_refs:
            wide = x_ref[...].astype(f32)
            total = total + jnp.sum(wide * wide, axis=-1, keepdims=True)
        scale = lax.rsqrt(total / dims + epsilon)
        t = order_ref[count + 1]
        for j, x_ref in enumerate(x_refs):
            first = (t ^ j) * per_piece if n_x > 1 else 0
            for b in range(per_piece):
                wide = x_ref[:, b * half : (b + 1) * half].astype(f32)
                xs[first + b] = (wide * scale * gain_ref[first + b]).astype(bf16)
        grp = order_ref[count]
        sums = []
        for j in range(3):
            src = order_ref[0]
            acc = jnp.dot(xs[2 * src], own_refs[j][0, :half], preferred_element_type=f32)
            acc += jnp.dot(xs[2 * src + 1], own_refs[j][0, half:], preferred_element_type=f32)
            for k in range(n_p):
                src = order_ref[k // 2 + 1]
                part = grp if k % 2 == 0 else 1 - grp
                acc += jnp.dot(xs[2 * src + part], piece_refs[3 * k + j][...], preferred_element_type=f32)
            sums.append(acc)
        q_ref[...] = head_norm(sums[0], qg_ref[...], head_size).astype(bf16)
        kv_ref[:, :width] = head_norm(sums[1], kg_ref[...], head_size).astype(bf16)
        kv_ref[:, width:] = sums[2].astype(bf16)

    return call(
        kernel, order, operands, specs,
        [jax.ShapeDtypeStruct((rows, width), bf16), jax.ShapeDtypeStruct((rows, 2 * width), bf16)],
        [pltpu.VMEM((blocks, rows, half), bf16)],
    )


def attend_kernel(query, kv_parts, doc_col, doc_row, flat_bias, order, count, head_size):
    rows, width = query.shape
    reach = LEFT * SEG
    span = reach + rows
    depth = len(kv_parts) - 1
    extent = flat_bias.shape[-1]
    operands = [query] + list(kv_parts) + [doc_col, doc_row, flat_bias]
    specs = [full_spec(a) for a in operands]

    def kernel(order_ref, q_ref, *refs):
        kv_refs, refs = refs[: depth + 1], refs[depth + 1 :]
        dc_ref, dr_ref, fb_ref, out_ref = refs
        offset = order_ref[0] * rows
        seg_q = lax.broadcasted_iota(jnp.int32, (rows, span), 0) // SEG
        col = lax.broadcasted_iota(jnp.int32, (rows, span), 1)
        seg_k = col // SEG - LEFT
        allowed = (
            (seg_k <= seg_q) & (seg_k >= seg_q - LEFT) & (col >= reach - offset)
            & (dc_ref[...] == dr_ref[...])
        )
        outs = []
        for h in range(width // head_size):
            lo = h * head_size
            keys = jnp.concatenate([r[:, lo : lo + head_size] for r in kv_refs], axis=0)
            vals = jnp.concatenate([r[:, width + lo : width + lo + head_size] for r in kv_refs], axis=0)
            scores = lax.dot_general(
                q_ref[:, lo : lo + head_size], keys, (((1,), (1,)), ((), ())),
                preferred_element_type=f32,
            ) * head_size ** (-0.5)
            line = jnp.broadcast_to(fb_ref[h], (rows, extent))
            bias = pltpu.roll(line, 0, 1, stride=1, stride_axis=0)[:, :span]
            scores = jnp.where(allowed, scores + bias, -1e30)
            peak = jnp.max(scores, axis=-1, keepdims=True)
            expo = jnp.exp(scores - peak)
            weights = (expo / jnp.sum(expo, axis=-1, keepdims=True)).astype(bf16)
            outs.append(jnp.dot(weights, vals, preferred_element_type=f32))
        out_ref[...] = jnp.concatenate(outs, axis=1).astype(bf16)

    return call(kernel, order, operands, specs, [jax.ShapeDtypeStruct((rows, width), bf16)], [])[0]


def output(attended, residual, own, layer, pieces, order, count):
    rows, dims = attended.shape
    half = own.shape[1] // 2
    cols = own.shape[2]
    blocks = dims // half
    operands = [attended, residual, own] + list(pieces)
    specs = [full_spec(attended), full_spec(residual)]
    specs += [window_spec((1, 2 * half, cols), (layer, 0, 0))] + [full_spec(p) for p in pieces]

    def kernel(order_ref, a_ref, r_ref, own_ref, *refs):
        piece_refs, (out_ref, xs) = refs[: len(pieces)], refs[len(pieces) :]
        for b in range(blocks):
            xs[b] = a_ref[:, b * half : (b + 1) * half]
        grp = order_ref[count]
        src = order_ref[0]
        acc = jnp.dot(xs[2 * src], own_ref[0, :half], preferred_element_type=f32)
        acc += jnp.dot(xs[2 * src + 1], own_ref[0, half:], preferred_element_type=f32)
        for k in range(len(pieces)):
            src = order_ref[k // 2 + 1]
            part = grp if k % 2 == 0 else 1 - grp
            acc += jnp.dot(xs[2 * src + part], piece_refs[k][...], preferred_element_type=f32)
        out_ref[...] = (r_ref[...].astype(f32) + acc).astype(bf16)

    return call(
        kernel, order, operands, specs, [jax.ShapeDtypeStruct((rows, cols), bf16)],
        [pltpu.VMEM((blocks, rows, half), bf16)],
    )[0]


def assemble(pieces, order, count):
    rows, cols = pieces[0].shape

    def kernel(order_ref, *refs):
        t = order_ref[count + 1]
        for j in range(len(pieces)):
            start = pl.multiple_of((t ^ j) * cols, cols)
            refs[-1][:, pl.ds(start, cols)] = refs[j][...]

    return call(
        kernel, order, pieces, [full_spec(a) for a in pieces],
        [jax.ShapeDtypeStruct((rows, cols * len(pieces)), bf16)], [],
    )[0]


def flat_biases(rel_bias, rows):
    reach = LEFT * SEG
    heads_here = rel_bias.shape[0]
    extent = 128 * (-(-(reach + 2 * rows - 1) // 128))
    far = jnp.broadcast_to(rel_bias[:, -1:], (heads_here, reach - MAXREL))
    near = rel_bias[:, MAXREL - rows + 1 :][:, ::-1]
    tail = jnp.broadcast_to(rel_bias[:, -1:], (heads_here, extent - reach - rows))
    return jnp.concatenate([far, near, tail], axis=1)[:, None, :]


def interleave(ring_pieces, group_pieces):
    return [p for pair in zip(ring_pieces, group_pieces) for p in pair]


def on_device_fast(
    stream, doc_ids, norm_gain, query_weight, key_weight, value_weight, out_weight,
    query_gain, key_gain, rel_bias,
):
    rows = stream.shape[0]
    count = lax.axis_size("sp")
    tp_count = lax.axis_size("tp")
    grp = lax.axis_index("grp")
    place = lax.axis_index("sp")
    t = lax.axis_index("tp")
    head_size = query_gain.shape[1]
    reach = LEFT * SEG
    depth = -(-reach // rows)
    cols = out_weight.shape[2]
    ring = folded_ring(count)
    slots = jnp.array([ring.index(i) for i in range(count)], jnp.int32)
    ring_of = jnp.array(ring, jnp.int32)
    steps = jnp.arange(count, dtype=jnp.int32)
    sources = ring_of[(slots[place] - steps) % count]
    order = jnp.concatenate([sources, jnp.stack([grp, t]).astype(jnp.int32)])

    in_half = query_weight.shape[1] // 2
    out_half = out_weight.shape[1] // 2

    def half_of(weight, size):
        return lax.dynamic_slice_in_dim(weight, grp * size, size, 0)

    def joined(layer):
        shards = (query_weight, key_weight, value_weight)
        return jnp.concatenate([half_of(w[layer], in_half) for w in shards], axis=1)

    first = joined(0)
    a_ring, a_group = [ring_step(first, ring)], []
    second = joined(1)
    out_halves = [half_of(out_weight[l], out_half) for l in range(LAYERS)]
    second = tie(second, a_ring[0])
    out_halves = [tie(h, a_ring[0]) for h in out_halves]
    docs = [tie(doc_ids, a_ring[0])]
    docs = [shifted(docs[0], "sp", back) for back in range(depth, 0, -1)] + docs
    for step in range(1, count - 1):
        source = tie(a_ring[-1], *a_group[-1:], *(docs if step > 1 else [second]))
        a_group.append(swap_groups(a_ring[-1]))
        a_ring.append(ring_step(source, ring))
    last, base = a_ring[-1], a_group[-1]
    a_group.append(swap_groups(tie(last, base)))
    c_ring, c_group = [ring_step(tie(second, last, base), ring)], []
    o_ring, o_group = [ring_step(tie(out_halves[0], last, base), ring)], []
    doc_row = jnp.concatenate(docs)[None, :]
    doc_col = doc_ids[:, None]
    flat = flat_biases(rel_bias, rows)

    residual = tie(lax.dynamic_slice_in_dim(stream, t * cols, cols, 1), a_ring[0])
    x_pieces = [stream]
    weights = (query_weight, key_weight, value_weight)
    for layer in range(LAYERS):
        ring_pieces, group_pieces = (a_ring, a_group) if layer == 0 else (c_ring, c_group)
        ahead = o_ring + c_ring[:1] if layer == 0 else o_ring
        query, kv = project(
            x_pieces, norm_gain[layer], query_gain[layer][None], key_gain[layer][None],
            weights, layer, interleave(ring_pieces, group_pieces), tie(order, *ahead), count,
        )
        received = [shifted(kv, "sp", 1)]
        o_group.append(swap_groups(tie(o_ring[-1], kv)))
        beside = [o_group[-1]]
        if layer == 0:
            c_group.append(swap_groups(tie(c_ring[0], kv)))
            beside.append(c_group[-1])
        for _ in range(depth - 1):
            received.insert(0, shifted(tie(received[0], beside[0]), "sp", 1))
        o_ring.append(ring_step(tie(o_ring[-1], received[-1], beside[0]), ring))
        attend_order = tie(order, o_ring[-1], *beside)
        middle = [tie(o_ring[-1], received[0])]
        o_group.append(swap_groups(middle[0]))
        o_ring.append(ring_step(middle[0], ring))
        if layer == 0:
            c_ring.append(ring_step(tie(c_ring[0], received[0], o_ring[1]), ring))
        attended = attend_kernel(
            query, received + [kv], doc_col, doc_row, flat, attend_order, count, head_size
        )
        attended = tie(attended, o_ring[-1], o_group[-1])
        o_group.append(swap_groups(tie(o_ring[-1], attended)))
        all_heads = lax.all_gather(attended, "tp", axis=1, tiled=True)
        out_order = order
        if layer == 0:
            out_order = tie(order, c_ring[-1])
            c_group.append(swap_groups(tie(c_ring[-1], all_heads)))
            c_ring.append(ring_step(tie(c_ring[-1], all_heads), ring))
        block = output(
            all_heads, residual, out_weight, layer, interleave(o_ring, o_group), out_order, count
        )
        x_pieces = exchange_columns(block, tp_count)
        if layer == 0:
            c_group.append(swap_groups(c_ring[-1]))
            o_ring, o_group = [ring_step(tie(out_halves[1], c_ring[-1]), ring)], []
        residual = block
    return assemble(x_pieces, order, count)


def on_device(*arrays):
    stream, query_weight, out_weight = arrays[0], arrays[3], arrays[6]
    rows, dims = stream.shape
    count, tp_count = lax.axis_size("sp"), lax.axis_size("tp")
    in_rows, width = query_weight.shape[1:]
    out_rows, cols = out_weight.shape[1:]
    fits = (
        lax.axis_size("grp") == 2 and LAYERS == 2
        and count == 4 and tp_count & (tp_count - 1) == 0
        and in_rows % 256 == 0 and out_rows % 256 == 0
        and 2 * (out_rows // 2) == in_rows // 2
        and width % 128 == 0 and cols % (2 * width) == 0
        and cols % (in_rows // 2) == 0 and tp_count > 1
        and rows <= MAXREL and (LEFT * SEG) % rows == 0 and rows % SEG == 0
    )
    return on_device_fast(*arrays) if fits else on_device_general(*arrays)


def solution(mesh):
    placed = (
        P(("grp", "sp"), None),
        P(("grp", "sp")),
        P(),
        P(None, "sp", "tp"),
        P(None, "sp", "tp"),
        P(None, "sp", "tp"),
        P(None, "sp", "tp"),
        P(),
        P(),
        P("tp", None),
    )
    return jax.shard_map(
        on_device, mesh=mesh, in_specs=placed, out_specs=P(("grp", "sp"), None), check_vma=False
    )
```

```python
import jax
import jax.numpy as jnp
from jax import lax
from jax.experimental import pallas as pl
from jax.experimental.pallas import tpu as pltpu
from jax.sharding import PartitionSpec as P

SEG = 64
LEFT = 8
MAXREL = 256
LAYERS = 2


epsilon = 1e-06


def shifted(value, axis, steps):
    count = lax.axis_size(axis)
    initial, last = (max(0, -steps), min(count, count - steps))
    return lax.ppermute(value, axis, [(source, source + steps) for source in range(initial, last)])


def row_norm(values, gain):
    return values * lax.rsqrt(jnp.mean(values * values, axis=-1, keepdims=True) + epsilon) * gain


def bias_table(rel_bias):
    heads_here = rel_bias.shape[0]
    reach = LEFT * SEG
    width = (LEFT + 1) * SEG
    highest = reach + SEG - 1
    reversed_bias = rel_bias[:, ::-1]
    upper_fill = jnp.broadcast_to(rel_bias[:, -1:], (heads_here, highest - MAXREL))
    flat_row = jnp.concatenate([upper_fill, reversed_bias[:, : MAXREL + SEG]], axis=1)
    lines = [
        flat_row[:, SEG - 1 - position : SEG - 1 - position + width] for position in range(SEG)
    ]
    return jnp.stack(lines, axis=1)


def attend(query, ext_keys, ext_values, ext_docs, own_docs, offset, table):
    rows, heads_here, head_size = query.shape
    count = rows // SEG
    width = (LEFT + 1) * SEG
    blocks = query.reshape(count, SEG, heads_here, head_size)
    key_blocks = ext_keys.reshape(count + LEFT, SEG, heads_here, head_size)
    value_blocks = ext_values.reshape(count + LEFT, SEG, heads_here, head_size)
    doc_blocks = ext_docs.reshape(count + LEFT, SEG)
    score_parts = [
        jnp.einsum(
            "nqhd,nkhd->nhqk",
            blocks,
            key_blocks[earlier : earlier + count],
            preferred_element_type=jnp.float32,
        )
        for earlier in range(LEFT + 1)
    ]
    scores = jnp.concatenate(score_parts, axis=-1)
    scores = scores * head_size ** (-0.5) + table[None]
    doc_band = jnp.concatenate(
        [doc_blocks[earlier : earlier + count] for earlier in range(LEFT + 1)], axis=1
    )
    key_pos = (
        offset
        + SEG * jnp.arange(count, dtype=jnp.int32)[:, None]
        - LEFT * SEG
        + jnp.arange(width, dtype=jnp.int32)[None, :]
    )
    allowed = (key_pos >= 0)[:, None, None, :] & (
        doc_band[:, None, None, :] == own_docs.reshape(count, SEG)[:, None, :, None]
    )
    scores = jnp.where(allowed, scores, -1e30)
    peak = jnp.max(scores, axis=-1, keepdims=True)
    expo = jnp.exp(scores - peak)
    weights = (expo / jnp.sum(expo, axis=-1, keepdims=True)).astype(jnp.bfloat16)
    mixed = jnp.zeros((count, SEG, heads_here, head_size), jnp.float32)
    for earlier in range(LEFT + 1):
        part_weights = weights[..., earlier * SEG : (earlier + 1) * SEG]
        mixed = mixed + jnp.einsum(
            "nhqk,nkhd->nqhd",
            part_weights,
            value_blocks[earlier : earlier + count],
            preferred_element_type=jnp.float32,
        )
    return mixed.astype(jnp.bfloat16).reshape(rows, heads_here * head_size)


def on_device_general(
    stream,
    doc_ids,
    norm_gain,
    query_weight,
    key_weight,
    value_weight,
    out_weight,
    query_gain,
    key_gain,
    rel_bias,
):
    rows = stream.shape[0]
    heads_here = rel_bias.shape[0]
    head_size = query_gain.shape[1]
    local_width = heads_here * head_size
    reach = LEFT * SEG
    depth = -(-reach // rows)
    offset = lax.axis_index("sp") * rows
    col_width = out_weight.shape[2]
    col_start = lax.axis_index("tp") * col_width
    table = bias_table(rel_bias)
    x = stream
    for layer in range(LAYERS):
        widened = x.astype(jnp.float32)
        normed = row_norm(widened, norm_gain[layer]).astype(jnp.bfloat16)
        own_cols = normed
        q_raw = jnp.dot(
            own_cols,
            lax.all_gather(query_weight[layer], "sp", axis=0, tiled=True),
            preferred_element_type=jnp.float32,
        )
        k_raw = jnp.dot(
            normed,
            lax.all_gather(key_weight[layer], "sp", axis=0, tiled=True),
            preferred_element_type=jnp.float32,
        )
        v_raw = jnp.dot(
            normed,
            lax.all_gather(value_weight[layer], "sp", axis=0, tiled=True),
            preferred_element_type=jnp.float32,
        )
        query = row_norm(q_raw.reshape(rows, heads_here, head_size), query_gain[layer]).astype(
            jnp.bfloat16
        )
        keys = row_norm(
            k_raw.reshape(normed.shape[0], heads_here, head_size), key_gain[layer]
        ).astype(jnp.bfloat16)
        values = v_raw.astype(jnp.bfloat16)
        flat_keys = keys.reshape(rows, local_width)
        tail = (flat_keys, values, doc_ids)
        received = [
            shifted((tail[0], tail[1], tail[2]), "sp", distance_back)
            for distance_back in range(depth, 0, -1)
        ]
        ext_keys = jnp.concatenate([item[0] for item in received] + [flat_keys], axis=0)
        ext_values = jnp.concatenate([item[1] for item in received] + [values], axis=0)
        ext_docs = jnp.concatenate([item[2] for item in received] + [doc_ids], axis=0)
        ext_keys = ext_keys.reshape(reach + rows, heads_here, head_size)
        ext_values = ext_values.reshape(reach + rows, heads_here, head_size)
        attended = attend(query, ext_keys, ext_values, ext_docs, doc_ids, offset, table)
        all_heads = lax.all_gather(attended, "tp", axis=1, tiled=True)
        projected = jnp.dot(
            all_heads,
            lax.all_gather(out_weight[layer], "sp", axis=0, tiled=True),
            preferred_element_type=jnp.float32,
        )
        own_cols = lax.dynamic_slice_in_dim(widened, col_start, col_width, 1)
        new_cols = (own_cols + projected).astype(jnp.bfloat16)
        x = lax.all_gather(new_cols, "tp", axis=1, tiled=True)
    return x


VMEM = pltpu.MemorySpace.VMEM
SMEM = pltpu.MemorySpace.SMEM
f32 = jnp.float32
bf16 = jnp.bfloat16


def folded_ring(count):
    return list(range(0, count, 2)) + list(range(1, count, 2))[::-1]


def ring_step(value, ring):
    count = len(ring)
    return lax.ppermute(value, "sp", [(ring[i], ring[(i + 1) % count]) for i in range(count)])


def tie(value, *others):
    return lax.optimization_barrier((value,) + others)[0]


def swap_groups(value):
    return lax.ppermute(value, "grp", [(0, 1), (1, 0)])


def exchange_columns(block, count):
    pieces = {0: block}
    step = count // 2
    while step:
        pairs = [(i, i ^ step) for i in range(count)]
        pieces.update({j ^ step: lax.ppermute(p, "tp", pairs) for j, p in list(pieces.items())})
        step //= 2
    return [pieces[j] for j in range(count)]


def full_spec(array):
    return pl.BlockSpec(array.shape, lambda i, n=array.ndim: (0,) * n)


def window_spec(shape, index):
    return pl.BlockSpec(shape, lambda i: index)


def call(kernel, order, operands, specs, out_shapes, scratch):
    return pl.pallas_call(
        kernel,
        grid=(1,),
        in_specs=[pl.BlockSpec(memory_space=SMEM)] + specs,
        out_specs=[pl.BlockSpec(o.shape, lambda i, n=len(o.shape): (0,) * n) for o in out_shapes],
        out_shape=out_shapes,
        scratch_shapes=scratch,
        compiler_params=pltpu.CompilerParams(vmem_limit_bytes=48 << 20),
    )(order, *operands)


def head_norm(raw, gain, head_size):
    parts = []
    for start in range(0, raw.shape[1], head_size):
        part = raw[:, start : start + head_size]
        parts.append(row_norm(part, gain))
    return jnp.concatenate(parts, axis=1)


def project(x_pieces, gain, q_gain, k_gain, own, layer, pieces, order, count):
    rows, piece_width = x_pieces[0].shape
    half = own[0].shape[1] // 2
    width = own[0].shape[2]
    dims = len(x_pieces) * piece_width
    blocks = dims // half
    per_piece = piece_width // half
    head_size = q_gain.shape[1]
    gain_blocks = gain.reshape(blocks, 1, half)
    operands = list(x_pieces) + [gain_blocks, q_gain, k_gain]
    specs = [full_spec(a) for a in operands]
    operands += list(own)
    specs += [window_spec((1, 2 * half, width), (layer, 0, 0)) for _ in own]
    for piece in pieces:
        for j in range(3):
            operands.append(piece)
            specs.append(window_spec((half, width), (0, j)))
    n_x, n_p = len(x_pieces), len(pieces)

    def kernel(order_ref, *refs):
        x_refs, refs = refs[:n_x], refs[n_x:]
        gain_ref, qg_ref, kg_ref = refs[:3]
        own_refs, refs = refs[3:6], refs[6:]
        piece_refs, refs = refs[: 3 * n_p], refs[3 * n_p :]
        q_ref, kv_ref, xs = refs
        total = jnp.zeros((rows, 1), f32)
        for x_ref in x_refs:
            wide = x_ref[...].astype(f32)
            total = total + jnp.sum(wide * wide, axis=-1, keepdims=True)
        scale = lax.rsqrt(total / dims + epsilon)
        t = order_ref[count + 1]
        for j, x_ref in enumerate(x_refs):
            first = (t ^ j) * per_piece if n_x > 1 else 0
            for b in range(per_piece):
                wide = x_ref[:, b * half : (b + 1) * half].astype(f32)
                xs[first + b] = (wide * scale * gain_ref[first + b]).astype(bf16)
        grp = order_ref[count]
        sums = []
        for j in range(3):
            src = order_ref[0]
            acc = jnp.dot(xs[2 * src], own_refs[j][0, :half], preferred_element_type=f32)
            acc += jnp.dot(xs[2 * src + 1], own_refs[j][0, half:], preferred_element_type=f32)
            for k in range(n_p):
                src = order_ref[k // 2 + 1]
                part = grp if k % 2 == 0 else 1 - grp
                acc += jnp.dot(xs[2 * src + part], piece_refs[3 * k + j][...], preferred_element_type=f32)
            sums.append(acc)
        q_ref[...] = head_norm(sums[0], qg_ref[...], head_size).astype(bf16)
        kv_ref[:, :width] = head_norm(sums[1], kg_ref[...], head_size).astype(bf16)
        kv_ref[:, width:] = sums[2].astype(bf16)

    return call(
        kernel, order, operands, specs,
        [jax.ShapeDtypeStruct((rows, width), bf16), jax.ShapeDtypeStruct((rows, 2 * width), bf16)],
        [pltpu.VMEM((blocks, rows, half), bf16)],
    )


def attend_kernel(query, kv_parts, doc_col, doc_row, flat_bias, order, count, head_size):
    rows, width = query.shape
    reach = LEFT * SEG
    span = reach + rows
    depth = len(kv_parts) - 1
    extent = flat_bias.shape[-1]
    operands = [query] + list(kv_parts) + [doc_col, doc_row, flat_bias]
    specs = [full_spec(a) for a in operands]

    def kernel(order_ref, q_ref, *refs):
        kv_refs, refs = refs[: depth + 1], refs[depth + 1 :]
        dc_ref, dr_ref, fb_ref, out_ref = refs
        offset = order_ref[0] * rows
        seg_q = lax.broadcasted_iota(jnp.int32, (rows, span), 0) // SEG
        col = lax.broadcasted_iota(jnp.int32, (rows, span), 1)
        seg_k = col // SEG - LEFT
        allowed = (
            (seg_k <= seg_q) & (seg_k >= seg_q - LEFT) & (col >= reach - offset)
            & (dc_ref[...] == dr_ref[...])
        )
        outs = []
        for h in range(width // head_size):
            lo = h * head_size
            keys = jnp.concatenate([r[:, lo : lo + head_size] for r in kv_refs], axis=0)
            vals = jnp.concatenate([r[:, width + lo : width + lo + head_size] for r in kv_refs], axis=0)
            scores = lax.dot_general(
                q_ref[:, lo : lo + head_size], keys, (((1,), (1,)), ((), ())),
                preferred_element_type=f32,
            ) * head_size ** (-0.5)
            line = jnp.broadcast_to(fb_ref[h], (rows, extent))
            bias = pltpu.roll(line, 0, 1, stride=1, stride_axis=0)[:, :span]
            scores = jnp.where(allowed, scores + bias, -1e30)
            peak = jnp.max(scores, axis=-1, keepdims=True)
            expo = jnp.exp(scores - peak)
            weights = (expo / jnp.sum(expo, axis=-1, keepdims=True)).astype(bf16)
            outs.append(jnp.dot(weights, vals, preferred_element_type=f32))
        out_ref[...] = jnp.concatenate(outs, axis=1).astype(bf16)

    return call(kernel, order, operands, specs, [jax.ShapeDtypeStruct((rows, width), bf16)], [])[0]


def output(attended, residual, own, layer, pieces, order, count):
    rows, dims = attended.shape
    half = own.shape[1] // 2
    cols = own.shape[2]
    blocks = dims // half
    operands = [attended, residual, own] + list(pieces)
    specs = [full_spec(attended), full_spec(residual)]
    specs += [window_spec((1, 2 * half, cols), (layer, 0, 0))] + [full_spec(p) for p in pieces]

    def kernel(order_ref, a_ref, r_ref, own_ref, *refs):
        piece_refs, (out_ref, xs) = refs[: len(pieces)], refs[len(pieces) :]
        for b in range(blocks):
            xs[b] = a_ref[:, b * half : (b + 1) * half]
        grp = order_ref[count]
        src = order_ref[0]
        acc = jnp.dot(xs[2 * src], own_ref[0, :half], preferred_element_type=f32)
        acc += jnp.dot(xs[2 * src + 1], own_ref[0, half:], preferred_element_type=f32)
        for k in range(len(pieces)):
            src = order_ref[k // 2 + 1]
            part = grp if k % 2 == 0 else 1 - grp
            acc += jnp.dot(xs[2 * src + part], piece_refs[k][...], preferred_element_type=f32)
        out_ref[...] = (r_ref[...].astype(f32) + acc).astype(bf16)

    return call(
        kernel, order, operands, specs, [jax.ShapeDtypeStruct((rows, cols), bf16)],
        [pltpu.VMEM((blocks, rows, half), bf16)],
    )[0]


def assemble(pieces, order, count):
    rows, cols = pieces[0].shape

    def kernel(order_ref, *refs):
        t = order_ref[count + 1]
        for j in range(len(pieces)):
            start = pl.multiple_of((t ^ j) * cols, cols)
            refs[-1][:, pl.ds(start, cols)] = refs[j][...]

    return call(
        kernel, order, pieces, [full_spec(a) for a in pieces],
        [jax.ShapeDtypeStruct((rows, cols * len(pieces)), bf16)], [],
    )[0]


def flat_biases(rel_bias, rows):
    reach = LEFT * SEG
    heads_here = rel_bias.shape[0]
    extent = 128 * (-(-(reach + 2 * rows - 1) // 128))
    far = jnp.broadcast_to(rel_bias[:, -1:], (heads_here, reach - MAXREL))
    near = rel_bias[:, MAXREL - rows + 1 :][:, ::-1]
    tail = jnp.broadcast_to(rel_bias[:, -1:], (heads_here, extent - reach - rows))
    return jnp.concatenate([far, near, tail], axis=1)[:, None, :]


def interleave(ring_pieces, group_pieces):
    return [p for pair in zip(ring_pieces, group_pieces) for p in pair]


def on_device_fast(
    stream, doc_ids, norm_gain, query_weight, key_weight, value_weight, out_weight,
    query_gain, key_gain, rel_bias,
):
    rows = stream.shape[0]
    count = lax.axis_size("sp")
    tp_count = lax.axis_size("tp")
    grp = lax.axis_index("grp")
    place = lax.axis_index("sp")
    t = lax.axis_index("tp")
    head_size = query_gain.shape[1]
    reach = LEFT * SEG
    depth = -(-reach // rows)
    cols = out_weight.shape[2]
    ring = folded_ring(count)
    slots = jnp.array([ring.index(i) for i in range(count)], jnp.int32)
    ring_of = jnp.array(ring, jnp.int32)
    steps = jnp.arange(count, dtype=jnp.int32)
    sources = ring_of[(slots[place] - steps) % count]
    order = jnp.concatenate([sources, jnp.stack([grp, t]).astype(jnp.int32)])

    in_half = query_weight.shape[1] // 2
    out_half = out_weight.shape[1] // 2

    def half_of(weight, size):
        return lax.dynamic_slice_in_dim(weight, grp * size, size, 0)

    def joined(layer):
        shards = (query_weight, key_weight, value_weight)
        return jnp.concatenate([half_of(w[layer], in_half) for w in shards], axis=1)

    first = joined(0)
    a_ring, a_group = [ring_step(first, ring)], []
    second = joined(1)
    out_halves = [half_of(out_weight[l], out_half) for l in range(LAYERS)]
    second = tie(second, a_ring[0])
    out_halves = [tie(h, a_ring[0]) for h in out_halves]
    flat = tie(flat_biases(rel_bias, rows), a_ring[0])
    residual = tie(lax.dynamic_slice_in_dim(stream, t * cols, cols, 1), a_ring[0])
    small = (flat, order, out_halves[0], residual)
    for step in range(1, count - 1):
        source = tie(a_ring[-1], *a_group[-1:], *(small if step > 1 else [second]))
        a_group.append(swap_groups(a_ring[-1]))
        a_ring.append(ring_step(source, ring))
    last, base = a_ring[-1], a_group[-1]
    docs = [tie(doc_ids, a_ring[1])]
    docs = [shifted(docs[0], "sp", back) for back in range(depth, 0, -1)] + docs
    a_group.append(swap_groups(tie(last, base)))
    c_ring, c_group = [ring_step(tie(second, last, base), ring)], []
    o_ring, o_group = [ring_step(tie(out_halves[0], last, base), ring)], []
    doc_row = jnp.concatenate(docs)[None, :]
    doc_col = doc_ids[:, None]
    x_pieces = [stream]
    weights = (query_weight, key_weight, value_weight)
    for layer in range(LAYERS):
        ring_pieces, group_pieces = (a_ring, a_group) if layer == 0 else (c_ring, c_group)
        ahead = [*o_ring, c_ring[0], doc_row, doc_col] if layer == 0 else o_ring
        query, kv = project(
            x_pieces, norm_gain[layer], query_gain[layer][None], key_gain[layer][None],
            weights, layer, interleave(ring_pieces, group_pieces), tie(order, *ahead), count,
        )
        received = [shifted(kv, "sp", 1)]
        o_group.append(swap_groups(tie(o_ring[-1], kv)))
        beside = [o_group[-1]]
        if layer == 0:
            c_group.append(swap_groups(tie(c_ring[0], kv)))
            beside.append(c_group[-1])
        for _ in range(depth - 1):
            received.insert(0, shifted(tie(received[0], beside[0]), "sp", 1))
        o_ring.append(ring_step(tie(o_ring[-1], received[-1], beside[0]), ring))
        attend_order = tie(order, o_ring[-1], *beside)
        middle = [tie(o_ring[-1], received[0])]
        o_group.append(swap_groups(middle[0]))
        o_ring.append(ring_step(middle[0], ring))
        if layer == 0:
            c_ring.append(ring_step(tie(c_ring[0], received[0], o_ring[1]), ring))
        attended = attend_kernel(
            query, received + [kv], doc_col, doc_row, flat, attend_order, count, head_size
        )
        attended = tie(attended, o_ring[-1], o_group[-1])
        o_group.append(swap_groups(tie(o_ring[-1], attended)))
        all_heads = lax.all_gather(attended, "tp", axis=1, tiled=True)
        out_order = order
        if layer == 0:
            out_order = tie(order, c_ring[-1])
            c_group.append(swap_groups(tie(c_ring[-1], all_heads)))
            c_ring.append(ring_step(tie(c_ring[-1], all_heads), ring))
        block = output(
            all_heads, residual, out_weight, layer, interleave(o_ring, o_group), out_order, count
        )
        x_pieces = exchange_columns(block, tp_count)
        if layer == 0:
            c_group.append(swap_groups(c_ring[-1]))
            o_ring, o_group = [ring_step(tie(out_halves[1], c_ring[-1]), ring)], []
        residual = block
    return assemble(x_pieces, order, count)


def on_device(*arrays):
    stream, query_weight, out_weight = arrays[0], arrays[3], arrays[6]
    rows, dims = stream.shape
    count, tp_count = lax.axis_size("sp"), lax.axis_size("tp")
    in_rows, width = query_weight.shape[1:]
    out_rows, cols = out_weight.shape[1:]
    fits = (
        lax.axis_size("grp") == 2 and LAYERS == 2
        and count == 4 and tp_count & (tp_count - 1) == 0
        and in_rows % 256 == 0 and out_rows % 256 == 0
        and 2 * (out_rows // 2) == in_rows // 2
        and width % 128 == 0 and cols % (2 * width) == 0
        and cols % (in_rows // 2) == 0 and tp_count > 1
        and rows <= MAXREL and (LEFT * SEG) % rows == 0 and rows % SEG == 0
    )
    return on_device_fast(*arrays) if fits else on_device_general(*arrays)


def solution(mesh):
    placed = (
        P(("grp", "sp"), None),
        P(("grp", "sp")),
        P(),
        P(None, "sp", "tp"),
        P(None, "sp", "tp"),
        P(None, "sp", "tp"),
        P(None, "sp", "tp"),
        P(),
        P(),
        P("tp", None),
    )
    return jax.shard_map(
        on_device, mesh=mesh, in_specs=placed, out_specs=P(("grp", "sp"), None), check_vma=False
    )
```
